32 devices in a mesh: sp: 8 (over z, y), fs: 2 (over x), tp: 2 (over core).
Axes of the slice: x: 2, y: 2, z: 4, core: 2. Of those that a mesh axis runs over, the one named last changes fastest.
Arguments:
- tokens: bfloat16 [8192, 2048], P(('fs', 'sp', 'tp')), parts along dimension 0, may hold values from -60 to 60
- norm_gain: float32 [2048], replicated, may hold values from 0.1 to 1.9
- pool_in: bfloat16 [2048, 512], P('sp', 'tp'), may hold values from -0.125 to 0.125
- gate_in: bfloat16 [2048, 1024], P('sp', 'tp'), may hold values from -0.125 to 0.125
- value_in: bfloat16 [2048, 1024], P('sp', 'tp'), may hold values from -0.125 to 0.125
- pool_mix: bfloat16 [4, 128, 128], P('tp'), may hold values from -0.5 to 0.5
- averaging_factor: float32 [512], P('tp'), may hold values from 0.25 to 0.75
- conv_taps: float32 [4, 1024], P(None, 'tp'), may hold values from -3 to 3
- rate_mix: bfloat16 [16, 64, 64], P('tp'), may hold values from -0.75 to 0.75
- input_mix: bfloat16 [16, 64, 64], P('tp'), may hold values from -0.75 to 0.75
- log_rate: float32 [1024], P('tp'), may hold values from 1.5 to 16
- decay_shift: float32 [32, 4096], P(('fs', 'tp'), 'sp'), parts along dimension 0, may hold values from -1.1 to 0
- initial_state: float32 [2048], P(('fs', 'tp')), parts along dimension 0, may hold values from -6 to 6
- out_pool: bfloat16 [2048, 512], P('sp', 'tp'), may hold values from -0.15625 to 0.15625
- out_rnn: bfloat16 [2048, 1024], P('sp', 'tp'), may hold values from -0.15625 to 0.15625
Outputs:
- mixed: bfloat16 [8192, 2048], P(('fs', 'sp', 'tp')), parts along dimension 0
The draws below stay inside these ranges and needn't reach their ends.
There are 2 independent parts, one for each index of `fs`. The reference program is written for one: setup_inputs(seed, part) draws one part's arguments, and reference() takes and returns one part's arrays. A program takes and returns all parts, laid end to end along the dimension named above; an argument that names none is the same for every part. Nothing has to cross between parts.
All inputs are finite; a program needn't handle non-finite values.
Results may differ from the reference program's by a relative error of at most 0.012.
Values may be sent and summed in bfloat16 or wider, within the bound.
No kernel may reach another device: no remote copies, remote signals or barrier semaphores. Data moves between devices by JAX's collectives and lax.ppermute only.
A program may use at most 64 MiB of HBM per device.

```python
import math
import jax
import jax.numpy as jnp
from jax import lax

D = 2048
POOL = 512
GROUPS = 4
GROUP_WIDTH = 128
LOOP_BRANCHES = 16
HEAD_DIM = 64
RNN = 1024
TAPS = 4
REACH = 16
TOK_DEV = 512
TOKEN_COUNT = 4096


def draw_tokens(key, part):
    derived_seed_list = jax.random.split(key, 3)
    row_scales = jnp.exp(jax.random.uniform(derived_seed_list[0], (TOKEN_COUNT, 1), jnp.float32, math.log(0.5), math.log(5.0)))
    column_scales = jnp.exp(jax.random.uniform(derived_seed_list[1], (1, D), jnp.float32, math.log(0.3), math.log(3.0)))
    entries = jax.random.truncated_normal(derived_seed_list[2], -4.0, 4.0, (TOKEN_COUNT, D), jnp.float32)
    return (entries * row_scales * column_scales).astype(jnp.bfloat16)


def draw_log_rate(key, part):
    derived_seed_list = jax.random.split(key, 3)
    chance = 0.5
    fast_heads = jax.random.bernoulli(derived_seed_list[0], chance, (LOOP_BRANCHES,))
    fast_rate = jax.random.uniform(derived_seed_list[1], (RNN,), jnp.float32, 2.0, 4.0) / TOK_DEV
    slow_rate = jax.random.uniform(derived_seed_list[2], (RNN,), jnp.float32, 0.04, 0.12) / TOKEN_COUNT
    per_channel = jnp.repeat(fast_heads, HEAD_DIM)
    step_rate = jnp.where(per_channel, fast_rate, slow_rate)
    return -jnp.log(jnp.expm1(step_rate))


def draw_decay_shift(key, part):
    derived_seed_list = jax.random.split(key, 3)
    blocks = TOKEN_COUNT // TOK_DEV
    block_level = jnp.exp(jax.random.uniform(derived_seed_list[0], (LOOP_BRANCHES, blocks), jnp.float32, math.log(0.1), math.log(2.0))) / TOKEN_COUNT
    steady_signal = -jnp.repeat(block_level, TOK_DEV, axis=1)
    cluster_indices = jax.random.randint(derived_seed_list[1], (LOOP_BRANCHES, 2, 1), 0, TOKEN_COUNT)
    loss_values = jax.random.uniform(derived_seed_list[2], (LOOP_BRANCHES, 2, 1), jnp.float32, 0.2, 0.4)
    match_tests = jnp.arange(TOKEN_COUNT, dtype=jnp.int32)[None, None, :] == cluster_indices
    spike_events = jnp.sum(jnp.where(match_tests, jnp.log1p(-loss_values), 0.0), axis=1)
    return steady_signal + spike_events


def shard_levels(key, shape, cuts, smallest, largest):
    level, own = 1.0, jax.random.fold_in(key, 6)
    for axis_at, parts in cuts:
        draws = jnp.exp(jax.random.uniform(jax.random.fold_in(own, axis_at), (parts,), jnp.float32, smallest / len(cuts), largest / len(cuts)))
        level = level * jnp.repeat(draws, shape[axis_at] // parts).reshape([-1 if axis == axis_at else 1 for axis in range(len(shape))])
    return level


def centred(own_key, shape, width, bound, cuts=(), kind=jnp.bfloat16):
    result = width * jax.random.normal(own_key, shape, jnp.float32)
    if cuts:
        result = result * shard_levels(own_key, shape, cuts, -0.22, 0.18)
    return jnp.clip(result, -bound, bound).astype(kind)


def setup_inputs(seed: int = 0, part: int = 0) -> dict:
    arg_keys = jax.random.split(jax.random.key(seed), 16)
    part_keys = jax.random.split(jax.random.fold_in(arg_keys[15], part), 16)
    tokens = draw_tokens(jax.random.fold_in(jax.random.fold_in(arg_keys[15], part), 71), part)
    norm_gain = jnp.clip(1.0 + 0.18 * jax.random.normal(arg_keys[1], (D,), jnp.float32), 0.1, 1.9)
    pool_in = centred(arg_keys[2], (D, POOL), D ** -0.5, 0.125, ((0, 8), (1, 2)))
    gate_in = centred(arg_keys[3], (D, RNN), D ** -0.5, 0.125, ((0, 8), (1, 2)))
    value_in = centred(arg_keys[4], (D, RNN), D ** -0.5, 0.125, ((0, 8), (1, 2)))
    pool_mix = centred(arg_keys[5], (GROUPS, GROUP_WIDTH, GROUP_WIDTH), GROUP_WIDTH ** -0.5, 0.5, ((0, 2),))
    averaging_factor = jnp.clip(0.25 + 0.5 * jax.random.uniform(arg_keys[6], (POOL,), jnp.float32) ** shard_levels(arg_keys[6], (POOL,), ((0, 2),), -0.2, 0.2), 0.25, 0.75)
    conv_taps = centred(arg_keys[7], (TAPS, RNN), TAPS ** -0.5, 3.0, ((1, 2),), jnp.float32)
    rate_mix = centred(arg_keys[8], (LOOP_BRANCHES, HEAD_DIM, HEAD_DIM), HEAD_DIM ** -0.5, 0.75, ((0, 2),))
    input_mix = centred(arg_keys[9], (LOOP_BRANCHES, HEAD_DIM, HEAD_DIM), HEAD_DIM ** -0.5, 0.75, ((0, 2),))
    log_rate = draw_log_rate(jax.random.fold_in(arg_keys[15], 71), part)
    decay_shift = draw_decay_shift(jax.random.fold_in(jax.random.fold_in(arg_keys[15], part), 71), part)
    initial_state = centred(part_keys[12], (RNN,), 1.0, 6.0, ((0, 2),), jnp.float32)
    out_pool = centred(arg_keys[13], (D, POOL), (POOL + RNN) ** -0.5, 0.15625, ((0, 8), (1, 2)))
    out_rnn = centred(arg_keys[14], (D, RNN), (POOL + RNN) ** -0.5, 0.15625, ((0, 8), (1, 2)))
    return {"tokens": tokens, "norm_gain": norm_gain, "pool_in": pool_in, "gate_in": gate_in, "value_in": value_in, "pool_mix": pool_mix, "averaging_factor": averaging_factor, "conv_taps": conv_taps, "rate_mix": rate_mix, "input_mix": input_mix, "log_rate": log_rate, "decay_shift": decay_shift, "initial_state": initial_state, "out_pool": out_pool, "out_rnn": out_rnn}


epsilon = 1e-06
sharpness = 8.0

def chain_pairs(first_pair, second_pair):
    return (first_pair[0] * second_pair[0], second_pair[0] * first_pair[1] + second_pair[1])

def reference(tokens, norm_gain, pool_in, gate_in, value_in, pool_mix, averaging_factor, conv_taps, rate_mix, input_mix, log_rate, decay_shift, initial_state, out_pool, out_rnn):
    widened = tokens.astype(jnp.float32)
    scaling = lax.rsqrt(lax.optimization_barrier(jnp.mean(widened * widened, axis=1, keepdims=True)) + epsilon)
    normed = (widened * scaling * norm_gain[None, :]).astype(jnp.bfloat16)
    pool_pre = jnp.dot(normed, pool_in, preferred_element_type=jnp.float32).astype(jnp.bfloat16)
    gate_pre = jnp.dot(normed, gate_in, preferred_element_type=jnp.float32).astype(jnp.bfloat16)
    value_pre = jnp.dot(normed, value_in, preferred_element_type=jnp.float32).astype(jnp.bfloat16)
    pool_values = pool_pre.astype(jnp.float32)
    pool_padded = jnp.pad(pool_values, ((REACH, 0), (0, 0)))
    positions = jnp.arange(TOKEN_COUNT, dtype=jnp.int32)
    pieces = []
    for group_index in range(GROUPS):
        window = 2 ** (group_index + 1)
        low_column = group_index * GROUP_WIDTH
        high_column = low_column + GROUP_WIDTH
        window_sum = jnp.zeros((TOKEN_COUNT, GROUP_WIDTH), jnp.float32)
        for steps_back in range(window):
            window_sum = window_sum + pool_padded[REACH - steps_back:REACH - steps_back + TOKEN_COUNT, low_column:high_column]
        counts = jnp.minimum(positions + 1, window).astype(jnp.float32)[:, None]
        pieces.append(window_sum / counts - pool_values[:, low_column:high_column])
    pooled = jnp.concatenate(pieces, axis=1).astype(jnp.bfloat16)
    mixed_groups = jnp.einsum('tgc,gcd->tgd', pooled.reshape(TOKEN_COUNT, GROUPS, GROUP_WIDTH).astype(jnp.float32), pool_mix.astype(jnp.float32))
    pool_out = (mixed_groups.reshape(TOKEN_COUNT, POOL) * averaging_factor[None, :]).astype(jnp.bfloat16)
    value_padded = jnp.pad(value_pre.astype(jnp.float32), ((TAPS - 1, 0), (0, 0)))
    convolved = conv_taps[0][None, :] * value_padded[0:TOKEN_COUNT]
    for tap_index in range(1, TAPS):
        convolved = convolved + conv_taps[tap_index][None, :] * value_padded[tap_index:tap_index + TOKEN_COUNT]
    conv_out = convolved.astype(jnp.bfloat16)
    conv_heads = conv_out.reshape(TOKEN_COUNT, LOOP_BRANCHES, HEAD_DIM).astype(jnp.float32)
    rate_gate = jax.nn.sigmoid(jnp.einsum('thc,hcd->thd', conv_heads, rate_mix.astype(jnp.float32))).reshape(TOKEN_COUNT, RNN)
    input_gate = jax.nn.sigmoid(jnp.einsum('thc,hcd->thd', conv_heads, input_mix.astype(jnp.float32))).reshape(TOKEN_COUNT, RNN)
    shifts = jnp.broadcast_to(jnp.transpose(decay_shift)[:, :, None], (TOKEN_COUNT, LOOP_BRANCHES, HEAD_DIM)).reshape(TOKEN_COUNT, RNN)
    log_decay = -sharpness * rate_gate * jax.nn.softplus(-log_rate)[None, :] + shifts
    decays = jnp.exp(log_decay)
    drives = jnp.sqrt(-jnp.expm1(2.0 * log_decay)) * input_gate * conv_out.astype(jnp.float32)
    cumulative, local_state = lax.associative_scan(chain_pairs, (decays, drives), axis=0)
    hidden_state = local_state + cumulative * initial_state[None, :]
    rnn_out = (jax.nn.gelu(gate_pre.astype(jnp.float32), approximate=True) * hidden_state).astype(jnp.bfloat16)
    pool_term = jnp.dot(pool_out, jnp.transpose(out_pool), preferred_element_type=jnp.float32)
    rnn_term = jnp.dot(rnn_out, jnp.transpose(out_rnn), preferred_element_type=jnp.float32)
    return (pool_term + rnn_term).astype(jnp.bfloat16)
```

```python
import jax
import jax.numpy as jnp
from jax import lax
from jax.experimental import pallas as pl
from jax.experimental.pallas import tpu as pltpu
from jax.sharding import PartitionSpec as P

GROUP_WIDTH = 128
HEAD_DIM = 64
TAPS = 4
REACH = 16


epsilon = 1e-06
sharpness = 8.0


def from_behind(value, axis, steps):
    count = lax.axis_size(axis)
    first, last = (max(0, -steps), min(count, count - steps))
    return lax.ppermute(value, axis, [(source, source + steps) for source in range(first, last)])


def right_product(left_rows, weight_rows):
    return lax.dot_general(
        left_rows, weight_rows, (((1,), (1,)), ((), ())), preferred_element_type=jnp.float32
    )


SEGMENTS = 8


def ring_order(place, count):
    half = count // 2
    return jnp.where(place < half, 2 * place, 2 * (count - 1 - place) + 1)


def ring_place(index, count):
    return jnp.where(index % 2 == 0, index // 2, count - 1 - index // 2)


def ring_gather(block, axis):
    count, index = (lax.axis_size(axis), lax.axis_index(axis))
    half = count // 2
    order = [2 * p if p < half else 2 * (count - 1 - p) + 1 for p in range(count)]
    place = ring_place(index, count)
    onward = [(order[p], order[(p + 1) % count]) for p in range(count)]
    backward = [(order[p], order[(p - 1) % count]) for p in range(count)]
    rows = block.shape[0]
    full = jnp.zeros((rows * count, block.shape[1]), block.dtype)

    def put(full, part, source, offset):
        return lax.dynamic_update_slice(
            full, part, (ring_order(source % count, count) * rows + offset, 0)
        )

    full = put(full, block, place, 0)
    right = left = block
    for step in range(1, half):
        right = lax.ppermute(right, axis, onward)
        left = lax.ppermute(left, axis, backward)
        full = put(full, right, place - step + count, 0)
        full = put(full, left, place + step, 0)
    middle = rows // 2
    right = lax.ppermute(right[:middle], axis, onward)
    left = lax.ppermute(left[middle:], axis, backward)
    full = put(full, right, place - half + count, 0)
    return put(full, left, place + half, middle)


def one_minus_exp(x):
    series = 1.0
    for order in range(8, 1, -1):
        series = 1.0 + x * (1.0 / order) * series
    return jnp.where(x > -0.35, -x * series, 1.0 - jnp.exp(x))


def mixer_kernel(
    where_ref,
    pool_ref,
    value_ref,
    edge_pool_ref,
    edge_value_ref,
    pool_mix_ref,
    factor_ref,
    taps_ref,
    gates_ref,
    rate_ref,
    shift_ref,
    pool_out_ref,
    cum_ref,
    state_ref,
    end_ref,
):
    rows = pool_ref.shape[0]
    groups_here = pool_ref.shape[1] // GROUP_WIDTH
    positions = where_ref[1] * rows + lax.broadcasted_iota(jnp.int32, (rows, GROUP_WIDTH), 0)
    for g in range(groups_here):
        cols = slice(g * GROUP_WIDTH, (g + 1) * GROUP_WIDTH)
        window = jnp.left_shift(2, where_ref[0] * groups_here + g)
        own = pool_ref[:, cols].astype(jnp.float32)
        total = jnp.concatenate([edge_pool_ref[:, cols].astype(jnp.float32), own], axis=0)
        reach = 1
        while reach < REACH:
            total = total + jnp.where(reach < window, pltpu.roll(total, reach, 0), 0.0)
            reach *= 2
        counts = jnp.minimum(positions + 1, window).astype(jnp.float32)
        pooled = (total[REACH:] / counts - own).astype(jnp.bfloat16)
        mixed = jnp.dot(pooled, pool_mix_ref[g], preferred_element_type=jnp.float32)
        pool_out_ref[:, cols] = (mixed * factor_ref[:, cols]).astype(jnp.bfloat16)
    width = 2 * HEAD_DIM
    lanes = lax.broadcasted_iota(jnp.int32, (rows, width), 1)
    for p in range(value_ref.shape[1] // width):
        cols = slice(p * width, (p + 1) * width)
        padded = jnp.concatenate([edge_value_ref[:, cols], value_ref[:, cols]], axis=0).astype(
            jnp.float32
        )
        convolved = taps_ref[TAPS - 1 : TAPS, cols] * padded
        for tap in range(TAPS - 1):
            convolved = convolved + taps_ref[tap : tap + 1, cols] * pltpu.roll(
                padded, TAPS - 1 - tap, 0
            )
        conv_out = convolved[REACH:].astype(jnp.bfloat16)
        terms = jnp.dot(conv_out, gates_ref[p], preferred_element_type=jnp.float32)
        rate_gate = jax.nn.sigmoid(terms[:, :width])
        input_gate = jax.nn.sigmoid(terms[:, width:])
        shifts = jnp.where(
            lanes < HEAD_DIM, shift_ref[:, 2 * p : 2 * p + 1], shift_ref[:, 2 * p + 1 : 2 * p + 2]
        )
        log_decay = rate_gate * rate_ref[:, cols] + shifts
        cum_ref[p] = jnp.exp(log_decay)
        state_ref[p] = (
            jnp.sqrt(one_minus_exp(2.0 * log_decay)) * input_gate * conv_out.astype(jnp.float32)
        )
        length = rows // SEGMENTS

        def advance(t, carry):
            product, state = carry
            at = (p, pl.ds(t, SEGMENTS, stride=length), slice(None))
            decay = cum_ref[at]
            product = product * decay
            state = state * decay + state_ref[at]
            cum_ref[at] = product
            state_ref[at] = state
            return product, state

        start = (jnp.ones((SEGMENTS, width), jnp.float32), jnp.zeros((SEGMENTS, width), jnp.float32))
        product, state = lax.fori_loop(0, length, advance, start, unroll=8)
        end_product, end_state = product[:1], state[:1]
        for s in range(1, SEGMENTS):
            end_state = end_state * product[s : s + 1] + state[s : s + 1]
            end_product = end_product * product[s : s + 1]
        end_ref[0:1, cols] = end_product
        end_ref[1:2, cols] = end_state


def finish_kernel(where_ref, gate_ref, cum_ref, state_ref, ends_ref, initial_ref, out_ref):
    rows = gate_ref.shape[0]
    width = 2 * HEAD_DIM
    carried = initial_ref[...]
    for k in range(ends_ref.shape[0] // 2):
        after = carried * ends_ref[2 * k : 2 * k + 1] + ends_ref[2 * k + 1 : 2 * k + 2]
        carried = jnp.where(k < where_ref[1], after, carried)
    length = rows // SEGMENTS
    for p in range(cum_ref.shape[0]):
        cols = slice(p * width, (p + 1) * width)
        before = carried[:, cols]
        for s in range(SEGMENTS):
            span = slice(s * length, (s + 1) * length)
            hidden = state_ref[p, span] + cum_ref[p, span] * before
            gate = jax.nn.gelu(gate_ref[span, cols].astype(jnp.float32), approximate=True)
            out_ref[span, cols] = (gate * hidden).astype(jnp.bfloat16)
            before = hidden[length - 1 : length]


def shards(
    tokens,
    norm_gain,
    pool_in,
    gate_in,
    value_in,
    pool_mix,
    averaging_factor,
    conv_taps,
    rate_mix,
    input_mix,
    log_rate,
    decay_shift,
    initial_state,
    out_pool,
    out_rnn,
):
    tp_index = lax.axis_index("tp")
    sp_index = lax.axis_index("sp")
    where = jnp.stack([tp_index, sp_index]).astype(jnp.int32)
    weight_in = ring_gather(jnp.concatenate([pool_in, value_in, gate_in], axis=1), "sp")
    weight_out = ring_gather(jnp.concatenate([out_pool, out_rnn], axis=1), "sp")
    pool_width = pool_in.shape[1]
    rnn_width = gate_in.shape[1]
    widened = lax.all_gather(tokens, "tp", axis=0, tiled=True).astype(jnp.float32)
    scaling = lax.rsqrt(jnp.mean(widened * widened, axis=1, keepdims=True) + epsilon)
    normed = (widened * scaling * norm_gain[None, :]).astype(jnp.bfloat16)
    projected = jnp.dot(normed, weight_in, preferred_element_type=jnp.float32).astype(jnp.bfloat16)
    block_rows = projected.shape[0]
    front_width = pool_width + rnn_width
    pool_pre = projected[:, :pool_width]
    value_pre = projected[:, pool_width:front_width]
    gate_pre = projected[:, front_width:]
    earlier_rows = from_behind(projected[block_rows - REACH :, :front_width], "sp", 1)
    pairs = rnn_width // (2 * HEAD_DIM)

    def paired(mix):
        halves = mix.reshape(pairs, 2, HEAD_DIM, HEAD_DIM)
        zero = jnp.zeros_like(halves[:, 0])
        upper = jnp.concatenate([halves[:, 0], zero], axis=2)
        lower = jnp.concatenate([zero, halves[:, 1]], axis=2)
        return jnp.concatenate([upper, lower], axis=1)

    gates = jnp.concatenate([paired(rate_mix), paired(input_mix)], axis=2)
    rate = (-sharpness * jax.nn.softplus(-log_rate))[None, :]
    vmem = pl.BlockSpec(memory_space=pltpu.VMEM)
    smem = pl.BlockSpec(memory_space=pltpu.SMEM)
    pool_out, cumulative, local_state, ends = pl.pallas_call(
        mixer_kernel,
        out_shape=(
            jax.ShapeDtypeStruct((block_rows, pool_width), jnp.bfloat16),
            jax.ShapeDtypeStruct((pairs, block_rows, 2 * HEAD_DIM), jnp.float32),
            jax.ShapeDtypeStruct((pairs, block_rows, 2 * HEAD_DIM), jnp.float32),
            jax.ShapeDtypeStruct((2, rnn_width), jnp.float32),
        ),
        in_specs=[smem] + [vmem] * 10,
        out_specs=(vmem,) * 4,
        name="mixer",
    )(
        where,
        pool_pre,
        value_pre,
        earlier_rows[:, :pool_width],
        earlier_rows[:, pool_width:],
        pool_mix,
        averaging_factor[None, :],
        conv_taps,
        gates,
        rate,
        jnp.transpose(decay_shift),
    )
    all_ends = lax.all_gather(ends, "sp", axis=0, tiled=True)
    rnn_out = pl.pallas_call(
        finish_kernel,
        out_shape=jax.ShapeDtypeStruct((block_rows, rnn_width), jnp.bfloat16),
        in_specs=[smem] + [vmem] * 5,
        out_specs=vmem,
        name="finish",
    )(where, gate_pre, cumulative, local_state, all_ends, initial_state[None, :])
    partial = right_product(jnp.concatenate([pool_out, rnn_out], axis=1), weight_out)
    return lax.psum_scatter(partial, "tp", scatter_dimension=0, tiled=True).astype(jnp.bfloat16)


def solution(mesh):
    placed = (
        P(("fs", "sp", "tp"), None),
        P(),
        P("sp", "tp"),
        P("sp", "tp"),
        P("sp", "tp"),
        P("tp", None, None),
        P("tp"),
        P(None, "tp"),
        P("tp", None, None),
        P("tp", None, None),
        P("tp"),
        P(("fs", "tp"), "sp"),
        P(("fs", "tp")),
        P("sp", "tp"),
        P("sp", "tp"),
    )
    return jax.shard_map(
        shards, mesh=mesh, in_specs=placed, out_specs=P(("fs", "sp", "tp"), None), check_vma=False
    )
```

```python
import jax
import jax.numpy as jnp
from jax import lax
from jax.experimental import pallas as pl
from jax.experimental.pallas import tpu as pltpu
from jax.sharding import PartitionSpec as P

GROUP_WIDTH = 128
HEAD_DIM = 64
TAPS = 4
REACH = 16


epsilon = 1e-06
sharpness = 8.0


def from_behind(value, axis, steps):
    count = lax.axis_size(axis)
    first, last = (max(0, -steps), min(count, count - steps))
    return lax.ppermute(value, axis, [(source, source + steps) for source in range(first, last)])


def right_product(left_rows, weight_rows):
    return lax.dot_general(
        left_rows, weight_rows, (((1,), (1,)), ((), ())), preferred_element_type=jnp.float32
    )


SEGMENTS = 8


def ring_order(place, count):
    half = count // 2
    return jnp.where(place < half, 2 * place, 2 * (count - 1 - place) + 1)


def ring_place(index, count):
    return jnp.where(index % 2 == 0, index // 2, count - 1 - index // 2)


def ring_blocks(block, axis):
    count, index = (lax.axis_size(axis), lax.axis_index(axis))
    half = count // 2
    order = [2 * p if p < half else 2 * (count - 1 - p) + 1 for p in range(count)]
    place = ring_place(index, count)
    onward = [(order[p], order[(p + 1) % count]) for p in range(count)]
    backward = [(order[p], order[(p - 1) % count]) for p in range(count)]
    middle = block.shape[0] // 2
    arrived = [(block, place, 0)]
    right = left = block
    for step in range(1, half + 1):
        last = step == half
        right = lax.ppermute(right[:middle] if last else right, axis, onward)
        left = lax.ppermute(left[middle:] if last else left, axis, backward)
        arrived.append((right, place - step + count, 0))
        arrived.append((left, place + step, middle if last else 0))
    rows = block.shape[0]
    return [
        (part, ring_order(source % count, count) * rows + offset)
        for part, source, offset in arrived
    ]


def lane_aligned(blocks):
    if all(part.shape[0] % 128 == 0 for part, _ in blocks):
        return blocks
    rows = lax.axis_size("sp") * blocks[0][0].shape[0]
    full = jnp.zeros((rows, blocks[0][0].shape[1]), blocks[0][0].dtype)
    for part, start in blocks:
        full = lax.dynamic_update_slice(full, part, (start, 0))
    return [(full, jnp.zeros((), jnp.int32))]


def one_minus_exp(x):
    series = 1.0
    for order in range(8, 1, -1):
        series = 1.0 + x * (1.0 / order) * series
    return jnp.where(x > -0.35, -x * series, 1.0 - jnp.exp(x))


def mixer_kernel(
    where_ref,
    pool_ref,
    value_ref,
    edge_pool_ref,
    edge_value_ref,
    pool_mix_ref,
    factor_ref,
    taps_ref,
    gates_ref,
    rate_ref,
    shift_ref,
    pool_out_ref,
    cum_ref,
    state_ref,
    end_ref,
):
    rows = pool_ref.shape[0]
    groups_here = pool_ref.shape[1] // GROUP_WIDTH
    positions = where_ref[1] * rows + lax.broadcasted_iota(jnp.int32, (rows, GROUP_WIDTH), 0)
    for g in range(groups_here):
        cols = slice(g * GROUP_WIDTH, (g + 1) * GROUP_WIDTH)
        window = jnp.left_shift(2, where_ref[0] * groups_here + g)
        own = pool_ref[:, cols].astype(jnp.float32)
        total = jnp.concatenate([edge_pool_ref[:, cols].astype(jnp.float32), own], axis=0)
        reach = 1
        while reach < REACH:
            total = total + jnp.where(reach < window, pltpu.roll(total, reach, 0), 0.0)
            reach *= 2
        counts = jnp.minimum(positions + 1, window).astype(jnp.float32)
        pooled = (total[REACH:] / counts - own).astype(jnp.bfloat16)
        mixed = jnp.dot(pooled, pool_mix_ref[g], preferred_element_type=jnp.float32)
        pool_out_ref[:, cols] = (mixed * factor_ref[:, cols]).astype(jnp.bfloat16)
    width = 2 * HEAD_DIM
    lanes = lax.broadcasted_iota(jnp.int32, (rows, width), 1)
    for p in range(value_ref.shape[1] // width):
        cols = slice(p * width, (p + 1) * width)
        padded = jnp.concatenate([edge_value_ref[:, cols], value_ref[:, cols]], axis=0).astype(
            jnp.float32
        )
        convolved = taps_ref[TAPS - 1 : TAPS, cols] * padded
        for tap in range(TAPS - 1):
            convolved = convolved + taps_ref[tap : tap + 1, cols] * pltpu.roll(
                padded, TAPS - 1 - tap, 0
            )
        conv_out = convolved[REACH:].astype(jnp.bfloat16)
        terms = jnp.dot(conv_out, gates_ref[p], preferred_element_type=jnp.float32)
        rate_gate = jax.nn.sigmoid(terms[:, :width])
        input_gate = jax.nn.sigmoid(terms[:, width:])
        shifts = jnp.where(
            lanes < HEAD_DIM, shift_ref[:, 2 * p : 2 * p + 1], shift_ref[:, 2 * p + 1 : 2 * p + 2]
        )
        log_decay = rate_gate * rate_ref[:, cols] + shifts
        cum_ref[p] = jnp.exp(log_decay)
        state_ref[p] = (
            jnp.sqrt(one_minus_exp(2.0 * log_decay)) * input_gate * conv_out.astype(jnp.float32)
        )
        length = rows // SEGMENTS

        def advance(t, carry):
            product, state = carry
            at = (p, pl.ds(t, SEGMENTS, stride=length), slice(None))
            decay = cum_ref[at]
            product = product * decay
            state = state * decay + state_ref[at]
            cum_ref[at] = product
            state_ref[at] = state
            return product, state

        start = (jnp.ones((SEGMENTS, width), jnp.float32), jnp.zeros((SEGMENTS, width), jnp.float32))
        product, state = lax.fori_loop(0, length, advance, start, unroll=8)
        end_product, end_state = product[:1], state[:1]
        for s in range(1, SEGMENTS):
            end_state = end_state * product[s : s + 1] + state[s : s + 1]
            end_product = end_product * product[s : s + 1]
        end_ref[0:1, cols] = end_product
        end_ref[1:2, cols] = end_state


def exit_columns(out_ref, starts_ref, pool_rows, rnn_rows, blocks):
    pool_width = pool_rows.shape[1]
    contract = (((1,), (1,)), ((), ()))
    for k, block in enumerate(blocks):
        size = block.shape[0]
        at = pl.ds(pl.multiple_of(starts_ref[k], 128), size)
        total = lax.dot_general(
            pool_rows, block[:, :pool_width], contract, preferred_element_type=jnp.float32
        ) + lax.dot_general(
            rnn_rows, block[:, pool_width:], contract, preferred_element_type=jnp.float32
        )
        out_ref[:, at] = total.astype(out_ref.dtype)


def finish_kernel(where_ref, starts_ref, gate_ref, cum_ref, state_ref, carried_ref, pool_ref, *refs):
    blocks, (rnn_ref, away_ref) = refs[:-2], refs[-2:]
    rows = gate_ref.shape[0]
    width = 2 * HEAD_DIM
    length = rows // SEGMENTS
    for p in range(cum_ref.shape[0]):
        cols = slice(p * width, (p + 1) * width)
        before = carried_ref[:, cols]
        for s in range(SEGMENTS):
            span = slice(s * length, (s + 1) * length)
            hidden = state_ref[p, span] + cum_ref[p, span] * before
            gate = jax.nn.gelu(gate_ref[span, cols].astype(jnp.float32), approximate=True)
            rnn_ref[span, cols] = (gate * hidden).astype(jnp.bfloat16)
            before = hidden[length - 1 : length]
    half = rows // 2
    span = pl.ds(pl.multiple_of((1 - where_ref[0]) * half, 128), half)
    exit_columns(away_ref, starts_ref, pool_ref[span, :], rnn_ref[span, :], blocks)


def keep_kernel(where_ref, starts_ref, pool_ref, rnn_ref, *refs):
    blocks, out_ref = refs[:-1], refs[-1]
    half = pool_ref.shape[0] // 2
    span = pl.ds(pl.multiple_of(where_ref[0] * half, 128), half)
    exit_columns(out_ref, starts_ref, pool_ref[span, :], rnn_ref[span, :], blocks)


def shards(
    tokens,
    norm_gain,
    pool_in,
    gate_in,
    value_in,
    pool_mix,
    averaging_factor,
    conv_taps,
    rate_mix,
    input_mix,
    log_rate,
    decay_shift,
    initial_state,
    out_pool,
    out_rnn,
):
    tp_index = lax.axis_index("tp")
    sp_index = lax.axis_index("sp")
    where = jnp.stack([tp_index, sp_index]).astype(jnp.int32)
    swap = [(t, t ^ 1) for t in range(lax.axis_size("tp"))]
    blocks_in = ring_blocks(jnp.concatenate([pool_in, value_in, gate_in], axis=1), "sp")
    own_out = jnp.concatenate([out_pool, out_rnn], axis=1)
    own_out, last_right, last_left = lax.optimization_barrier(
        (own_out, blocks_in[-2][0], blocks_in[-1][0])
    )
    blocks_in[-2] = (last_right, blocks_in[-2][1])
    blocks_in[-1] = (last_left, blocks_in[-1][1])
    blocks_out = lane_aligned(ring_blocks(own_out, "sp"))
    pool_width = pool_in.shape[1]
    rnn_width = gate_in.shape[1]
    widened = tokens.astype(jnp.float32)
    scaling = lax.rsqrt(jnp.mean(widened * widened, axis=1, keepdims=True) + epsilon)
    normed_own = (widened * scaling * norm_gain[None, :]).astype(jnp.bfloat16)
    normed_peer = lax.ppermute(normed_own, "tp", swap)
    first = tp_index == 0
    normed = jnp.concatenate(
        [jnp.where(first, normed_own, normed_peer), jnp.where(first, normed_peer, normed_own)],
        axis=0,
    )
    summed = jnp.zeros((normed.shape[0], pool_width + 2 * rnn_width), jnp.float32)
    for part, start in blocks_in:
        columns = lax.dynamic_slice_in_dim(normed, start, part.shape[0], axis=1)
        summed = summed + jnp.dot(columns, part, preferred_element_type=jnp.float32)
    projected = summed.astype(jnp.bfloat16)
    block_rows = projected.shape[0]
    front_width = pool_width + rnn_width
    pool_pre = projected[:, :pool_width]
    value_pre = projected[:, pool_width:front_width]
    gate_pre = projected[:, front_width:]
    earlier_rows = from_behind(projected[block_rows - REACH :, :front_width], "sp", 1)
    pairs = rnn_width // (2 * HEAD_DIM)

    def paired(mix):
        halves = mix.reshape(pairs, 2, HEAD_DIM, HEAD_DIM)
        zero = jnp.zeros_like(halves[:, 0])
        upper = jnp.concatenate([halves[:, 0], zero], axis=2)
        lower = jnp.concatenate([zero, halves[:, 1]], axis=2)
        return jnp.concatenate([upper, lower], axis=1)

    gates = jnp.concatenate([paired(rate_mix), paired(input_mix)], axis=2)
    rate = (-sharpness * jax.nn.softplus(-log_rate))[None, :]
    vmem = pl.BlockSpec(memory_space=pltpu.VMEM)
    smem = pl.BlockSpec(memory_space=pltpu.SMEM)
    pool_out, cumulative, local_state, ends = pl.pallas_call(
        mixer_kernel,
        out_shape=(
            jax.ShapeDtypeStruct((block_rows, pool_width), jnp.bfloat16),
            jax.ShapeDtypeStruct((pairs, block_rows, 2 * HEAD_DIM), jnp.float32),
            jax.ShapeDtypeStruct((pairs, block_rows, 2 * HEAD_DIM), jnp.float32),
            jax.ShapeDtypeStruct((2, rnn_width), jnp.float32),
        ),
        in_specs=[smem] + [vmem] * 10,
        out_specs=(vmem,) * 4,
        name="mixer",
    )(
        where,
        pool_pre,
        value_pre,
        earlier_rows[:, :pool_width],
        earlier_rows[:, pool_width:],
        pool_mix,
        averaging_factor[None, :],
        conv_taps,
        gates,
        rate,
        jnp.transpose(decay_shift),
    )
    count = lax.axis_size("sp")
    through = ends
    reach = 1
    while reach < count:
        earlier = from_behind(through, "sp", reach)
        product = earlier[:1] * through[:1]
        state = through[:1] * earlier[1:] + through[1:]
        through = jnp.where(
            sp_index >= reach, jnp.concatenate([product, state], axis=0), through
        )
        reach *= 2
    initial = initial_state[None, :]
    reached = through[:1] * initial + through[1:]
    carried = jnp.where(sp_index == 0, initial, from_behind(reached, "sp", 1))
    out_parts = [part for part, _ in blocks_out]
    starts = jnp.stack([start for _, start in blocks_out]).astype(jnp.int32)
    half_rows = block_rows // 2
    features = own_out.shape[0] * count
    rnn_out, away = pl.pallas_call(
        finish_kernel,
        out_shape=(
            jax.ShapeDtypeStruct((block_rows, rnn_width), jnp.bfloat16),
            jax.ShapeDtypeStruct((half_rows, features), jnp.bfloat16),
        ),
        in_specs=[smem, smem] + [vmem] * (5 + len(out_parts)),
        out_specs=(vmem, vmem),
        name="finish",
    )(where, starts, gate_pre, cumulative, local_state, carried, pool_out, *out_parts)
    arriving = lax.ppermute(away, "tp", swap)
    kept = pl.pallas_call(
        keep_kernel,
        out_shape=jax.ShapeDtypeStruct((half_rows, features), jnp.float32),
        in_specs=[smem, smem] + [vmem] * (2 + len(out_parts)),
        out_specs=vmem,
        name="keep",
    )(where, starts, pool_out, rnn_out, *out_parts)
    return (kept + arriving.astype(jnp.float32)).astype(jnp.bfloat16)


def solution(mesh):
    placed = (
        P(("fs", "sp", "tp"), None),
        P(),
        P("sp", "tp"),
        P("sp", "tp"),
        P("sp", "tp"),
        P("tp", None, None),
        P("tp"),
        P(None, "tp"),
        P("tp", None, None),
        P("tp", None, None),
        P("tp"),
        P(("fs", "tp"), "sp"),
        P(("fs", "tp")),
        P("sp", "tp"),
        P("sp", "tp"),
    )
    return jax.shard_map(
        shards, mesh=mesh, in_specs=placed, out_specs=P(("fs", "sp", "tp"), None), check_vma=False
    )
```

```python
import jax
import jax.numpy as jnp
from jax import lax
from jax.experimental import pallas as pl
from jax.experimental.pallas import tpu as pltpu
from jax.sharding import PartitionSpec as P

GROUP_WIDTH = 128
HEAD_DIM = 64
TAPS = 4
REACH = 16


epsilon = 1e-06
sharpness = 8.0


def from_behind(value, axis, steps):
    count = lax.axis_size(axis)
    first, last = (max(0, -steps), min(count, count - steps))
    return lax.ppermute(value, axis, [(source, source + steps) for source in range(first, last)])


SEGMENTS = 8


def ring_order(place, count):
    half = count // 2
    return jnp.where(place < half, 2 * place, 2 * (count - 1 - place) + 1)


def ring_place(index, count):
    return jnp.where(index % 2 == 0, index // 2, count - 1 - index // 2)


def ring_blocks(block, axis):
    count, index = (lax.axis_size(axis), lax.axis_index(axis))
    half = count // 2
    order = [2 * p if p < half else 2 * (count - 1 - p) + 1 for p in range(count)]
    place = ring_place(index, count)
    onward = [(order[p], order[(p + 1) % count]) for p in range(count)]
    backward = [(order[p], order[(p - 1) % count]) for p in range(count)]
    middle = block.shape[0] // 2
    arrived = [(block, place, 0)]
    right = left = block
    for step in range(1, half + 1):
        last = step == half
        right = lax.ppermute(right[:middle] if last else right, axis, onward)
        left = lax.ppermute(left[middle:] if last else left, axis, backward)
        arrived.append((right, place - step + count, 0))
        arrived.append((left, place + step, middle if last else 0))
    rows = block.shape[0]
    return [
        (part, ring_order(source % count, count) * rows + offset)
        for part, source, offset in arrived
    ]


def lane_aligned(blocks):
    if all(part.shape[0] % 128 == 0 for part, _ in blocks):
        return blocks
    rows = lax.axis_size("sp") * blocks[0][0].shape[0]
    full = jnp.zeros((rows, blocks[0][0].shape[1]), blocks[0][0].dtype)
    for part, start in blocks:
        full = lax.dynamic_update_slice(full, part, (start, 0))
    return [(full, jnp.zeros((), jnp.int32))]


def one_minus_exp(x):
    series = 1.0
    for order in range(8, 1, -1):
        series = 1.0 + x * (1.0 / order) * series
    return jnp.where(x > -0.35, -x * series, 1.0 - jnp.exp(x))


def mixer_kernel(
    where_ref,
    pool_ref,
    value_ref,
    edge_pool_ref,
    edge_value_ref,
    pool_mix_ref,
    factor_ref,
    taps_ref,
    gates_ref,
    rate_ref,
    shift_ref,
    pool_out_ref,
    cum_ref,
    state_ref,
    end_ref,
):
    rows = pool_ref.shape[0]
    groups_here = pool_ref.shape[1] // GROUP_WIDTH
    positions = where_ref[1] * rows + lax.broadcasted_iota(jnp.int32, (rows, GROUP_WIDTH), 0)
    for g in range(groups_here):
        cols = slice(g * GROUP_WIDTH, (g + 1) * GROUP_WIDTH)
        window = jnp.left_shift(2, where_ref[0] * groups_here + g)
        own = pool_ref[:, cols].astype(jnp.float32)
        total = jnp.concatenate([edge_pool_ref[:, cols].astype(jnp.float32), own], axis=0)
        reach = 1
        while reach < REACH:
            total = total + jnp.where(reach < window, pltpu.roll(total, reach, 0), 0.0)
            reach *= 2
        counts = jnp.minimum(positions + 1, window).astype(jnp.float32)
        pooled = (total[REACH:] / counts - own).astype(jnp.bfloat16)
        mixed = jnp.dot(pooled, pool_mix_ref[g], preferred_element_type=jnp.float32)
        pool_out_ref[:, cols] = (mixed * factor_ref[:, cols]).astype(jnp.bfloat16)
    width = 2 * HEAD_DIM
    lanes = lax.broadcasted_iota(jnp.int32, (rows, width), 1)
    for p in range(value_ref.shape[1] // width):
        cols = slice(p * width, (p + 1) * width)
        padded = jnp.concatenate([edge_value_ref[:, cols], value_ref[:, cols]], axis=0).astype(
            jnp.float32
        )
        convolved = taps_ref[TAPS - 1 : TAPS, cols] * padded
        for tap in range(TAPS - 1):
            convolved = convolved + taps_ref[tap : tap + 1, cols] * pltpu.roll(
                padded, TAPS - 1 - tap, 0
            )
        conv_out = convolved[REACH:].astype(jnp.bfloat16)
        terms = jnp.dot(conv_out, gates_ref[p], preferred_element_type=jnp.float32)
        rate_gate = jax.nn.sigmoid(terms[:, :width])
        input_gate = jax.nn.sigmoid(terms[:, width:])
        shifts = jnp.where(
            lanes < HEAD_DIM, shift_ref[:, 2 * p : 2 * p + 1], shift_ref[:, 2 * p + 1 : 2 * p + 2]
        )
        log_decay = rate_gate * rate_ref[:, cols] + shifts
        cum_ref[p] = jnp.exp(log_decay)
        state_ref[p] = (
            jnp.sqrt(one_minus_exp(2.0 * log_decay)) * input_gate * conv_out.astype(jnp.float32)
        )
        length = rows // SEGMENTS

        def advance(t, carry):
            product, state = carry
            at = (p, pl.ds(t, SEGMENTS, stride=length), slice(None))
            decay = cum_ref[at]
            product = product * decay
            state = state * decay + state_ref[at]
            cum_ref[at] = product
            state_ref[at] = state
            return product, state

        start = (jnp.ones((SEGMENTS, width), jnp.float32), jnp.zeros((SEGMENTS, width), jnp.float32))
        product, state = lax.fori_loop(0, length, advance, start, unroll=8)
        end_product, end_state = product[:1], state[:1]
        for s in range(1, SEGMENTS):
            end_state = end_state * product[s : s + 1] + state[s : s + 1]
            end_product = end_product * product[s : s + 1]
        end_ref[0:1, cols] = end_product
        end_ref[1:2, cols] = end_state


def exit_columns(out_ref, starts_ref, pool_rows, rnn_rows, blocks):
    pool_width = pool_rows.shape[1]
    contract = (((1,), (1,)), ((), ()))
    for k, block in enumerate(blocks):
        size = block.shape[0]
        at = pl.ds(pl.multiple_of(starts_ref[k], 128), size)
        total = lax.dot_general(
            pool_rows, block[:, :pool_width], contract, preferred_element_type=jnp.float32
        ) + lax.dot_general(
            rnn_rows, block[:, pool_width:], contract, preferred_element_type=jnp.float32
        )
        out_ref[:, at] = total.astype(out_ref.dtype)


def finish_kernel(where_ref, starts_ref, gate_ref, cum_ref, state_ref, carried_ref, pool_ref, *refs):
    blocks, (rnn_ref, away_ref) = refs[:-2], refs[-2:]
    rows = gate_ref.shape[0]
    width = 2 * HEAD_DIM
    length = rows // SEGMENTS
    for p in range(cum_ref.shape[0]):
        cols = slice(p * width, (p + 1) * width)
        before = carried_ref[:, cols]
        for s in range(SEGMENTS):
            span = slice(s * length, (s + 1) * length)
            hidden = state_ref[p, span] + cum_ref[p, span] * before
            gate = jax.nn.gelu(gate_ref[span, cols].astype(jnp.float32), approximate=True)
            rnn_ref[span, cols] = (gate * hidden).astype(jnp.bfloat16)
            before = hidden[length - 1 : length]
    half = rows // 2
    span = pl.ds(pl.multiple_of((1 - where_ref[0]) * half, 128), half)
    exit_columns(away_ref, starts_ref, pool_ref[span, :], rnn_ref[span, :], blocks)


def keep_kernel(where_ref, starts_ref, pool_ref, rnn_ref, *refs):
    blocks, out_ref = refs[:-1], refs[-1]
    half = pool_ref.shape[0] // 2
    span = pl.ds(pl.multiple_of(where_ref[0] * half, 128), half)
    exit_columns(out_ref, starts_ref, pool_ref[span, :], rnn_ref[span, :], blocks)


def shards(
    tokens,
    norm_gain,
    pool_in,
    gate_in,
    value_in,
    pool_mix,
    averaging_factor,
    conv_taps,
    rate_mix,
    input_mix,
    log_rate,
    decay_shift,
    initial_state,
    out_pool,
    out_rnn,
):
    tp_index = lax.axis_index("tp")
    sp_index = lax.axis_index("sp")
    where = jnp.stack([tp_index, sp_index]).astype(jnp.int32)
    swap = [(t, t ^ 1) for t in range(lax.axis_size("tp"))]
    blocks_in = ring_blocks(jnp.concatenate([pool_in, value_in, gate_in], axis=1), "sp")
    own_out = jnp.concatenate([out_pool, out_rnn], axis=1)
    own_out, last_right, last_left = lax.optimization_barrier(
        (own_out, blocks_in[-2][0], blocks_in[-1][0])
    )
    blocks_in[-2] = (last_right, blocks_in[-2][1])
    blocks_in[-1] = (last_left, blocks_in[-1][1])
    blocks_out = lane_aligned(ring_blocks(own_out, "sp"))
    pool_width = pool_in.shape[1]
    rnn_width = gate_in.shape[1]
    widened = tokens.astype(jnp.float32)
    scaling = lax.rsqrt(jnp.mean(widened * widened, axis=1, keepdims=True) + epsilon)
    normed_own = (widened * scaling * norm_gain[None, :]).astype(jnp.bfloat16)
    normed_peer = lax.ppermute(normed_own, "tp", swap)
    first = tp_index == 0
    normed = jnp.concatenate(
        [jnp.where(first, normed_own, normed_peer), jnp.where(first, normed_peer, normed_own)],
        axis=0,
    )
    summed = jnp.zeros((normed.shape[0], pool_width + 2 * rnn_width), jnp.float32)
    for part, start in blocks_in:
        columns = lax.dynamic_slice_in_dim(normed, start, part.shape[0], axis=1)
        summed = summed + jnp.dot(columns, part, preferred_element_type=jnp.float32)
    projected = summed.astype(jnp.bfloat16)
    block_rows = projected.shape[0]
    front_width = pool_width + rnn_width
    pool_pre = projected[:, :pool_width]
    value_pre = projected[:, pool_width:front_width]
    gate_pre = projected[:, front_width:]
    earlier_rows = from_behind(projected[block_rows - REACH :, :front_width], "sp", 1)
    pairs = rnn_width // (2 * HEAD_DIM)

    def paired(mix):
        halves = mix.reshape(pairs, 2, HEAD_DIM, HEAD_DIM)
        zero = jnp.zeros_like(halves[:, 0])
        upper = jnp.concatenate([halves[:, 0], zero], axis=2)
        lower = jnp.concatenate([zero, halves[:, 1]], axis=2)
        return jnp.concatenate([upper, lower], axis=1)

    gates = jnp.concatenate([paired(rate_mix), paired(input_mix)], axis=2)
    rate = (-sharpness * jax.nn.softplus(-log_rate))[None, :]
    vmem = pl.BlockSpec(memory_space=pltpu.VMEM)
    smem = pl.BlockSpec(memory_space=pltpu.SMEM)
    pool_out, cumulative, local_state, ends = pl.pallas_call(
        mixer_kernel,
        out_shape=(
            jax.ShapeDtypeStruct((block_rows, pool_width), jnp.bfloat16),
            jax.ShapeDtypeStruct((pairs, block_rows, 2 * HEAD_DIM), jnp.float32),
            jax.ShapeDtypeStruct((pairs, block_rows, 2 * HEAD_DIM), jnp.float32),
            jax.ShapeDtypeStruct((2, rnn_width), jnp.float32),
        ),
        in_specs=[smem] + [vmem] * 10,
        out_specs=(vmem,) * 4,
        name="mixer",
    )(
        where,
        pool_pre,
        value_pre,
        earlier_rows[:, :pool_width],
        earlier_rows[:, pool_width:],
        pool_mix,
        averaging_factor[None, :],
        conv_taps,
        gates,
        rate,
        jnp.transpose(decay_shift),
    )
    count = lax.axis_size("sp")
    through = ends
    reach = 1
    while reach < count:
        earlier = from_behind(through, "sp", reach)
        product = earlier[:1] * through[:1]
        state = through[:1] * earlier[1:] + through[1:]
        through = jnp.where(
            sp_index >= reach, jnp.concatenate([product, state], axis=0), through
        )
        reach *= 2
    initial = initial_state[None, :]
    reached = through[:1] * initial + through[1:]
    behind = from_behind(reached, "sp", 1)
    carried = jnp.where(sp_index == 0, initial, behind)
    out_parts = [part for part, _ in blocks_out]
    starts = jnp.stack([start for _, start in blocks_out]).astype(jnp.int32)
    half_rows = block_rows // 2
    features = own_out.shape[0] * count
    rnn_out, away = pl.pallas_call(
        finish_kernel,
        out_shape=(
            jax.ShapeDtypeStruct((block_rows, rnn_width), jnp.bfloat16),
            jax.ShapeDtypeStruct((half_rows, features), jnp.bfloat16),
        ),
        in_specs=[smem, smem] + [vmem] * (5 + len(out_parts)),
        out_specs=(vmem, vmem),
        name="finish",
    )(where, starts, gate_pre, cumulative, local_state, carried, pool_out, *out_parts)
    arriving = lax.ppermute(away, "tp", swap)
    kept = pl.pallas_call(
        keep_kernel,
        out_shape=jax.ShapeDtypeStruct((half_rows, features), jnp.float32),
        in_specs=[smem, smem] + [vmem] * (2 + len(out_parts)),
        out_specs=vmem,
        name="keep",
    )(where, starts, pool_out, rnn_out, *out_parts)
    return (kept + arriving.astype(jnp.float32)).astype(jnp.bfloat16)


def solution(mesh):
    placed = (
        P(("fs", "sp", "tp"), None),
        P(),
        P("sp", "tp"),
        P("sp", "tp"),
        P("sp", "tp"),
        P("tp", None, None),
        P("tp"),
        P(None, "tp"),
        P("tp", None, None),
        P("tp", None, None),
        P("tp"),
        P(("fs", "tp"), "sp"),
        P(("fs", "tp")),
        P("sp", "tp"),
        P("sp", "tp"),
    )

    return jax.shard_map(
        shards, mesh=mesh, in_specs=placed, out_specs=P(("fs", "sp", "tp"), None), check_vma=False
    )
```
